32 devices in a mesh: sp: 8 (over z, y), tp: 4 (over x, core).
Axes of the slice: x: 2, y: 2, z: 4, core: 2. Of those that a mesh axis runs over, the one named last changes fastest.
Arguments:
- block_input: bfloat16 [8192, 2048], P('sp'), may hold values from -6 to 6
- out_grad: bfloat16 [8192, 2048], P('sp'), may hold values from -6 to 6
- w_value: bfloat16 [2048, 1024], P(None, 'tp'), may hold values from -0.125 to 0.125
- w_gate: bfloat16 [2048, 1024], P(None, 'tp'), may hold values from -0.125 to 0.125
- conv_taps: float32 [31, 1024], P(None, 'tp'), may hold values from -4 to 4
- norm_gain: float32 [1024], P('tp'), may hold values from 0.1 to 1.9
- norm_shift: float32 [1024], P('tp'), may hold values from -3 to 3
- w_proj: bfloat16 [1024, 2048], P('tp'), may hold values from -0.1875 to 0.1875
Outputs:
- input_grad: bfloat16 [8192, 2048], P('sp', 'tp')
- value_wgrad: float32 [2048, 1024], P('sp', 'tp')
- gate_wgrad: float32 [2048, 1024], P('sp', 'tp')
- proj_wgrad: float32 [1024, 2048], P('tp', 'sp')
- taps_grad: float32 [31, 1024], P(None, 'tp')
- gain_grad: float32 [1024], P('tp')
- shift_grad: float32 [1024], P('tp')
The draws below stay inside these ranges and needn't reach their ends.
All inputs are finite; a program needn't handle non-finite values.
Results may differ from the reference program's by a relative error of at most 0.014.
Values may be sent and summed in bfloat16 or wider, within the bound.
A program may use at most 128 MiB of HBM per device.

```python
import math
import jax
import jax.numpy as jnp
from jax import lax

D = 2048
CH = 1024
KERNEL = 31
TOKENS = 8192
N_TP = 4


def draw_conv_taps(key, part):
    base = jax.random.fold_in(key, 11)
    first, second, third = jax.random.split(base, 3)
    channel = jnp.arange(CH, dtype=jnp.float32)
    phase = jax.random.uniform(first, (), jnp.float32, 0.0, 6.2831)
    level = jnp.exp(1.2 * jnp.sin(6.2831853 * channel / CH + phase))
    rough = jnp.exp(jax.random.uniform(second, (CH,), jnp.float32, -0.7, 0.7))
    taps = jax.random.truncated_normal(third, -3.0, 3.0, (KERNEL, CH), jnp.float32)
    return (taps * (level * rough)[None, :] / math.sqrt(KERNEL)).astype(jnp.float32)


def with_spikes(entries, rng, source, target, parts, factor):
    def block_of(dim):
        return (jnp.arange(entries.shape[dim]) // (entries.shape[dim] // parts)).reshape((-1,) + (1,) * (entries.ndim - 1 - dim))

    one_side = jax.random.permutation(rng, parts)[block_of(target)]
    other_side = (block_of(target) + parts // 2) % parts
    return jnp.where((block_of(source) == one_side) | (block_of(source) == other_side), factor * entries, entries)


def shard_levels(rng, dims, cuts, low, top_value):
    def one(dim, shards_of):
        steps = jax.random.uniform(jax.random.fold_in(jax.random.fold_in(rng, 6), dim), (shards_of,), jnp.float32, low / len(cuts), top_value / len(cuts))
        return jnp.repeat(jnp.exp(steps), dims[dim] // shards_of).reshape((-1,) + (1,) * (len(dims) - dim - 1))

    gain = one(*cuts[0])
    for cut in cuts[1:]:
        gain = gain * one(*cut)
    return gain


def scatter_about(stream_key, dims, spread, reach, pieces=(), kind=jnp.bfloat16):
    result = spread * jax.random.normal(stream_key, dims, jnp.float32)
    if pieces:
        result = result * shard_levels(stream_key, dims, pieces, -0.22, 0.18)
    return jnp.clip(result, -reach, reach).astype(kind)


def gaussian_with(own_key, dims, scale, limit, cuts, heavy, kind=jnp.bfloat16):
    entries = scale * jax.random.normal(own_key, dims, jnp.float32)
    if cuts:
        entries = entries * shard_levels(own_key, dims, cuts, -0.22, 0.18)
    return jnp.clip(with_spikes(entries, jax.random.fold_in(own_key, 3), *heavy), -limit, limit).astype(kind)


def setup_inputs(seed: int = 0) -> dict:
    streams_of = jax.random.split(jax.random.key(seed), 9)
    block_input = scatter_about(streams_of[0], (TOKENS, D), 1.0, 6.0, ((0, 8),))
    out_grad = gaussian_with(streams_of[1], (TOKENS, D), 1.0, 6.0, ((0, 8),), (0, 1, 8, 2.0))
    w_value = scatter_about(streams_of[2], (D, CH), D ** -0.5, 0.125, ((1, 4),))
    w_gate = scatter_about(streams_of[3], (D, CH), D ** -0.5, 0.125, ((1, 4),))
    conv_taps = draw_conv_taps(jax.random.fold_in(streams_of[8], 71), 0)
    norm_gain = jnp.clip(1.0 + 0.18 * jax.random.normal(streams_of[5], (CH,), jnp.float32), 0.1, 1.9)
    norm_shift = scatter_about(streams_of[6], (CH,), 0.5, 3.0, ((0, 4),), jnp.float32)
    w_proj = scatter_about(streams_of[7], (CH, D), CH ** -0.5, 0.1875, ((0, 4),))
    return {"block_input": block_input, "out_grad": out_grad, "w_value": w_value, "w_gate": w_gate, "conv_taps": conv_taps, "norm_gain": norm_gain, "norm_shift": norm_shift, "w_proj": w_proj}


EPS = 0.05

def reference(block_input, out_grad, w_value, w_gate, conv_taps, norm_gain, norm_shift, w_proj):
    value_proj = jnp.dot(block_input, w_value, preferred_element_type=jnp.float32).astype(jnp.bfloat16)
    gate_proj = jnp.dot(block_input, w_gate, preferred_element_type=jnp.float32).astype(jnp.bfloat16)
    gate_sigmoid = jax.nn.sigmoid(gate_proj.astype(jnp.float32))
    value_wide = value_proj.astype(jnp.float32)
    gated_input = (value_wide * gate_sigmoid).astype(jnp.bfloat16)
    padded_glu = jnp.pad(gated_input.astype(jnp.float32), ((KERNEL - 1, 0), (0, 0)))
    filtered = jnp.zeros((TOKENS, CH), jnp.float32)
    for tap_index in range(KERNEL):
        begin = KERNEL - 1 - tap_index
        filtered = filtered + conv_taps[tap_index] * padded_glu[begin:begin + TOKENS]
    row_mean = lax.optimization_barrier(jnp.sum(filtered, axis=1)) / CH
    row_var = lax.optimization_barrier(jnp.sum(filtered * filtered, axis=1)) / CH - row_mean * row_mean
    row_scale = lax.rsqrt(row_var + EPS)
    normed = (filtered - row_mean[:, None]) * row_scale[:, None]
    activated = normed * norm_gain + norm_shift
    act_sigmoid = jax.nn.sigmoid(activated)
    mixer_out = (activated * act_sigmoid).astype(jnp.bfloat16)
    grad_mixed = jnp.dot(out_grad, w_proj.T, preferred_element_type=jnp.float32)
    grad_act = grad_mixed * act_sigmoid * (1.0 + activated * (1.0 - act_sigmoid))
    grad_normed = grad_act * norm_gain
    first_mean = lax.optimization_barrier(jnp.sum(grad_normed, axis=1)) / CH
    second_mean = lax.optimization_barrier(jnp.sum(grad_normed * normed, axis=1)) / CH
    grad_filtered = row_scale[:, None] * (grad_normed - first_mean[:, None] - normed * second_mean[:, None])
    padded_grad = jnp.pad(grad_filtered, ((0, KERNEL - 1), (0, 0)))
    grad_glu = jnp.zeros((TOKENS, CH), jnp.float32)
    taps_rows = []
    for tap_index in range(KERNEL):
        begin = KERNEL - 1 - tap_index
        grad_glu = grad_glu + conv_taps[tap_index] * padded_grad[tap_index:tap_index + TOKENS]
        taps_rows.append(lax.optimization_barrier(jnp.sum(grad_filtered * padded_glu[begin:begin + TOKENS], axis=0)))
    grad_value = (grad_glu * gate_sigmoid).astype(jnp.bfloat16)
    grad_gate = (grad_glu * value_wide * gate_sigmoid * (1.0 - gate_sigmoid)).astype(jnp.bfloat16)
    block_cols = CH // N_TP
    summed = jnp.zeros((TOKENS, D), jnp.float32)
    for block_index in range(N_TP):
        low = block_index * block_cols
        high = low + block_cols
        partial_sum = jnp.dot(grad_value[:, low:high], w_value[:, low:high].T, preferred_element_type=jnp.float32)
        partial_sum = partial_sum + jnp.dot(grad_gate[:, low:high], w_gate[:, low:high].T, preferred_element_type=jnp.float32)
        summed = summed + partial_sum.astype(jnp.bfloat16).astype(jnp.float32)
    input_grad = summed.astype(jnp.bfloat16)
    loss_scale = 1.0 / jnp.sqrt(jnp.float32(TOKENS))
    value_wgrad = jnp.dot(block_input.T, grad_value, preferred_element_type=jnp.float32) * loss_scale
    gate_wgrad = jnp.dot(block_input.T, grad_gate, preferred_element_type=jnp.float32) * loss_scale
    proj_wgrad = jnp.dot(mixer_out.T, out_grad, preferred_element_type=jnp.float32) * loss_scale
    taps_grad = jnp.stack(taps_rows, axis=0) * loss_scale
    gain_grad = lax.optimization_barrier(jnp.sum(grad_act * normed, axis=0)) * loss_scale
    shift_grad = lax.optimization_barrier(jnp.sum(grad_act, axis=0)) * loss_scale
    return (input_grad, value_wgrad, gate_wgrad, proj_wgrad, taps_grad, gain_grad, shift_grad)
```

```python
import functools
import math

import jax
import jax.numpy as jnp
from jax import lax
from jax.experimental import pallas as pl
from jax.experimental.pallas import tpu as pltpu
from jax.sharding import PartitionSpec as P

CH = 1024


EPS = 0.05


def from_behind(block, axis, distance):
    devices = range(lax.axis_size(axis))
    route = [(i - distance, i) for i in devices if i - distance in devices]
    return lax.ppermute(block, axis, route)


def right_product(left, right):
    return lax.dot_general(
        left, right, (((1,), (1,)), ((), ())), preferred_element_type=jnp.float32
    )


def column_product(left, right):
    return lax.dot_general(
        left, right, (((0,), (0,)), ((), ())), preferred_element_type=jnp.float32
    )


MESH = pl.DeviceIdType.MESH


def tail_kernel(
    n, n_tp, loss_scale,
    bi_hbm, og_hbm, wv_hbm, wg_hbm, gb_ref, mo_ref, small_ref,
    ig_ref, ws_ref, ps_ref, sm_ref,
    bi, og, wv, wg,
    gs, gr, gs2, gq, pm, pr, ps2, pq,
    xs, xr, ys, yr, acc, small_pair, small_in, small_all,
    load_sem,
    gs_send, gs_recv, gq_send, gq_recv, pr_send, pr_recv, pq_send, pq_recv,
    x_send, x_recv, y_send, y_recv, s_send, s_recv, sa_send, sa_recv,
):
    me, t = lax.axis_index("sp"), lax.axis_index("tp")
    outer, inner = me // 2, me % 2
    h = n // 2
    mate = 2 * outer + (1 - inner)
    t_near, t_far = t + 1 - 2 * (t % 2), lax.rem(t + n_tp // 2, n_tp)
    t_cross = lax.rem(t_near + n_tp // 2, n_tp)
    rows = bi.shape[1] // n
    tokens = bi.shape[0]
    cols = bi.shape[1] // n_tp
    chans = mo_ref.shape[1]
    chunks = xs.shape[0]
    step = tokens // chunks

    loads = []
    for i, (src, dst) in enumerate(((bi_hbm, bi), (wv_hbm, wv), (wg_hbm, wg), (og_hbm, og))):
        loads.append(pltpu.make_async_copy(src, dst, load_sem.at[i]))
        loads[-1].start()

    barrier = pltpu.get_barrier_semaphore()
    peers = [{"sp": 2 * lax.rem(outer + k, h) + inner} for k in range(1, h)]
    for who in peers + [{"sp": mate}, {"tp": t_near}, {"tp": t_far}]:
        pl.semaphore_signal(barrier, inc=1, device_id=who, device_id_type=MESH)
    pl.semaphore_wait(barrier, len(peers) + 3)

    def send(src, dst, send_sem, recv_sem, who):
        copy = pltpu.make_async_remote_copy(
            src_ref=src, dst_ref=dst, send_sem=send_sem, recv_sem=recv_sem,
            device_id=who, device_id_type=MESH,
        )
        copy.start()
        return copy

    small_copy = send(small_ref, small_in, s_send.at[0], s_recv.at[0], {"sp": mate})

    aligned = rows % 128 == 0
    wide = 256
    def block_rows(o, i):
        return pl.ds(pl.multiple_of((2 * o + i) * rows, rows), rows)

    def product(act, other, where):
        return lax.dot_general(
            act[:, where], other[...], (((0,), (0,)), ((), ())),
            preferred_element_type=jnp.float32,
        ).astype(jnp.bfloat16)

    def make_block(store, act, other, o, i):
        if aligned:
            store[block_rows(o, i), :] = product(act, other, block_rows(o, i))

    def make_all(store, act, other):
        if not aligned:
            for c in range(act.shape[1] // wide):
                where = pl.ds(c * wide, wide)
                store[where, :] = product(act, other, where)

    def partial_input(r, j):
        at = pl.ds(pl.multiple_of(j * cols, cols), cols)
        token = pl.ds(r * step, step)
        return right_product(gb_ref[token, :chans], wv[at, :]) + right_product(
            gb_ref[token, chans:], wg[at, :]
        )

    order = [lax.rem(outer + k, h) for k in range(1, h)] + [outer]

    def near_block(r):
        xs[r, 0] = partial_input(r, t_near).astype(jnp.bfloat16)
        xs[r, 1] = partial_input(r, t_cross).astype(jnp.bfloat16)
        return send(xs.at[r], xr.at[r], x_send.at[r], x_recv.at[r], {"tp": t_near})

    def far_block(r):
        mine = partial_input(r, t)
        far = partial_input(r, t_far)
        x_copies[r].wait_recv()
        ys[r] = (far + xr[r, 1].astype(jnp.float32)).astype(jnp.bfloat16)
        acc[pl.ds(r * step, step), :] = mine + xr[r, 0].astype(jnp.float32)
        return send(ys.at[r], yr.at[r], y_send.at[r], y_recv.at[r], {"tp": t_far})

    loads[0].wait()
    make_all(gs, bi, gb_ref)
    g_copies = []
    x_copies = []
    y_copies = []

    def g_block(k):
        o = order[k]
        make_block(gs, bi, gb_ref, o, 1 - inner)
        where = block_rows(o, 1 - inner)
        g_copies.append(send(gs.at[where], gr.at[k], gs_send.at[k], gs_recv.at[k], {"sp": mate}))

    g_block(0)
    loads[1].wait()
    loads[2].wait()
    x_copies.append(near_block(0))
    g_block(1)
    x_copies.append(near_block(1))
    y_copies.append(far_block(0))
    loads[3].wait()
    make_all(pm, og, mo_ref)
    p_copies = []
    for k in range(h - 1):
        o = order[k]
        for i in range(2):
            make_block(pm, og, mo_ref, o, i)
        where = pl.ds(pl.multiple_of(2 * o * rows, 2 * rows), 2 * rows)
        p_copies.append(send(pm.at[where], pr.at[k], pr_send.at[k], pr_recv.at[k], {"sp": 2 * o + inner}))
        if k + 2 < h:
            g_block(k + 2)
    for r in range(2, chunks):
        x_copies.append(near_block(r))
        y_copies.append(far_block(r - 1))
    y_copies.append(far_block(chunks - 1))
    for i in range(2):
        make_block(pm, og, mo_ref, outer, i)
    small_copy.wait()
    small_pair[...] = small_ref[...] + small_in[...]
    sa_copies = [
        send(small_pair, small_all.at[outer], sa_send.at[k - 1], sa_recv.at[k - 1],
             {"sp": 2 * lax.rem(outer + k, h) + inner})
        for k in range(1, h)
    ]
    q_copies = []
    for k in range(h):
        o = order[k]
        make_block(gs, bi, gb_ref, o, inner)
        g_copies[k].wait_recv()
        total = gs[block_rows(o, inner), :].astype(jnp.float32) + gr[k].astype(jnp.float32)
        if k < h - 1:
            gs2[k] = total.astype(jnp.bfloat16)
            q_copies.append(send(gs2.at[k], gq.at[k], gq_send.at[k], gq_recv.at[k], {"sp": 2 * o + inner}))
        else:
            ws_ref[...] = total
    for copy in p_copies:
        copy.wait_recv()

    def proj_total(i):
        total = pm[block_rows(outer, i), :].astype(jnp.float32)
        for k in range(h - 1):
            total = total + pr[k, pl.ds(pl.multiple_of(i * rows, rows), rows), :].astype(jnp.float32)
        return total

    ps2[...] = proj_total(1 - inner).astype(jnp.bfloat16)
    last = send(ps2, pq, pq_send.at[0], pq_recv.at[0], {"sp": mate})
    ps_ref[...] = proj_total(inner)
    for copy in sa_copies:
        copy.wait_recv()
    small_all[outer] = small_pair[...]
    total = small_all[0]
    for k in range(1, h):
        total = total + small_all[k]
    sm_ref[...] = total * loss_scale
    for r in range(chunks):
        y_copies[r].wait_recv()
        token = pl.ds(r * step, step)
        ig_ref[token, :] = (acc[token, :] + yr[r].astype(jnp.float32)).astype(jnp.bfloat16)
    for copy in q_copies:
        copy.wait_recv()
    total = ws_ref[...]
    for k in range(h - 1):
        total = total + gq[k].astype(jnp.float32)
    ws_ref[...] = total * loss_scale
    last.wait_recv()
    ps_ref[...] = (ps_ref[...] + pq[...].astype(jnp.float32)) * loss_scale
    for copy in g_copies + x_copies + y_copies + p_copies + q_copies + sa_copies + [last]:
        copy.wait_send()


def tail(block_input, out_grad, w_value, w_gate, grad_both, mixer_out, small, loss_scale):
    n, n_tp = lax.axis_size("sp"), lax.axis_size("tp")
    tokens, width = block_input.shape
    chans = mixer_out.shape[1]
    rows, cols, h, chunks = width // n, width // n_tp, n // 2, 4
    step = tokens // chunks
    bf, f32 = jnp.bfloat16, jnp.float32
    anywhere = pl.BlockSpec(memory_space=pl.ANY)
    vmem = pl.BlockSpec(memory_space=pltpu.VMEM)
    dma = pltpu.SemaphoreType.DMA
    V = pltpu.VMEM
    return pl.pallas_call(
        functools.partial(tail_kernel, n, n_tp, loss_scale),
        out_shape=(
            jax.ShapeDtypeStruct((tokens, cols), bf),
            jax.ShapeDtypeStruct((rows, 2 * chans), f32),
            jax.ShapeDtypeStruct((rows, chans), f32),
            jax.ShapeDtypeStruct(small.shape, f32),
        ),
        in_specs=[anywhere] * 4 + [vmem] * 3,
        out_specs=(vmem,) * 4,
        scratch_shapes=[
            V((tokens, width), bf), V((tokens, width), bf), V((width, chans), bf), V((width, chans), bf),
            V((width, 2 * chans), bf), V((h, rows, 2 * chans), bf), V((h - 1, rows, 2 * chans), bf),
            V((h - 1, rows, 2 * chans), bf),
            V((width, chans), bf), V((h - 1, 2 * rows, chans), bf), V((rows, chans), bf), V((rows, chans), bf),
            V((chunks, 2, step, cols), bf), V((chunks, 2, step, cols), bf), V((chunks, step, cols), bf),
            V((chunks, step, cols), bf), V((tokens, cols), f32),
            V(small.shape, f32), V(small.shape, f32), V((h,) + small.shape, f32),
            dma((4,)),
            dma((h,)), dma((h,)), dma((h - 1,)), dma((h - 1,)), dma((h - 1,)), dma((h - 1,)), dma((1,)), dma((1,)),
            dma((chunks,)), dma((chunks,)), dma((chunks,)), dma((chunks,)), dma((1,)), dma((1,)),
            dma((h - 1,)), dma((h - 1,)),
        ],
        compiler_params=pltpu.CompilerParams(
            collective_id=0, has_side_effects=True, vmem_limit_bytes=60 * 1024 * 1024
        ),
    )(block_input, out_grad, w_value, w_gate, grad_both, mixer_out, small)


def shards(block_input, out_grad, w_value, w_gate, conv_taps, norm_gain, norm_shift, w_proj):
    tok_rows = block_input.shape[0]
    kernel_len = conv_taps.shape[0]
    reach_back = kernel_len - 1
    channels_dev = w_value.shape[1]
    loss_scale = 1.0 / math.sqrt(tok_rows * lax.axis_size("sp"))
    value_proj = jnp.dot(block_input, w_value, preferred_element_type=jnp.float32).astype(
        jnp.bfloat16
    )
    gate_proj = jnp.dot(block_input, w_gate, preferred_element_type=jnp.float32).astype(
        jnp.bfloat16
    )
    gate_sigmoid = jax.nn.sigmoid(gate_proj.astype(jnp.float32))
    value_wide = value_proj.astype(jnp.float32)
    gated_input = (value_wide * gate_sigmoid).astype(jnp.bfloat16)
    earlier = from_behind(gated_input[tok_rows - reach_back :], "sp", 1)
    extended = jnp.concatenate([earlier, gated_input], axis=0).astype(jnp.float32)
    filtered = jnp.zeros((tok_rows, channels_dev), jnp.float32)
    for tap_index in range(kernel_len):
        begin = reach_back - tap_index
        filtered = filtered + conv_taps[tap_index] * extended[begin : begin + tok_rows]
    row_sum, row_square = lax.psum(
        (jnp.sum(filtered, axis=1), jnp.sum(filtered * filtered, axis=1)), "tp"
    )
    row_mean = row_sum / CH
    row_var = row_square / CH - row_mean * row_mean
    row_scale = lax.rsqrt(row_var + EPS)
    normed = (filtered - row_mean[:, None]) * row_scale[:, None]
    activated = normed * norm_gain + norm_shift
    act_sigmoid = jax.nn.sigmoid(activated)
    mixer_out = (activated * act_sigmoid).astype(jnp.bfloat16)
    grad_mixed = right_product(out_grad, w_proj)
    grad_act = grad_mixed * act_sigmoid * (1.0 + activated * (1.0 - act_sigmoid))
    grad_normed = grad_act * norm_gain
    back_sum, back_cross = lax.psum(
        (jnp.sum(grad_normed, axis=1), jnp.sum(grad_normed * normed, axis=1)), "tp"
    )
    grad_filtered = row_scale[:, None] * (
        grad_normed - back_sum[:, None] / CH - normed * (back_cross[:, None] / CH)
    )
    gain_part = jnp.sum(grad_act * normed, axis=0)
    shift_part = jnp.sum(grad_act, axis=0)
    padded_grad = jnp.pad(grad_filtered, ((reach_back, reach_back), (0, 0)))
    grad_extended = jnp.zeros((tok_rows + reach_back, channels_dev), jnp.float32)
    taps_rows = []
    for tap_index in range(kernel_len):
        begin = reach_back - tap_index
        grad_extended = (
            grad_extended
            + conv_taps[tap_index] * padded_grad[tap_index : tap_index + tok_rows + reach_back]
        )
        taps_rows.append(jnp.sum(grad_filtered * extended[begin : begin + tok_rows], axis=0))
    taps_part = jnp.stack(taps_rows, axis=0)
    returned = from_behind(grad_extended[:reach_back], "sp", -1)
    grad_glu = jnp.concatenate(
        [grad_extended[reach_back:tok_rows], grad_extended[tok_rows:] + returned], axis=0
    )
    grad_value = (grad_glu * gate_sigmoid).astype(jnp.bfloat16)
    grad_gate = (grad_glu * value_wide * gate_sigmoid * (1.0 - gate_sigmoid)).astype(jnp.bfloat16)
    grad_both = jnp.concatenate([grad_value, grad_gate], axis=1)
    small = jnp.concatenate([taps_part, gain_part[None], shift_part[None]], axis=0)
    small = jnp.pad(small, ((0, -small.shape[0] % 8), (0, 0)))
    input_grad, weight_sum, proj_sum, small_sum = tail(
        block_input, out_grad, w_value, w_gate, grad_both, mixer_out, small, loss_scale
    )
    return (
        input_grad,
        weight_sum[:, :channels_dev],
        weight_sum[:, channels_dev:],
        proj_sum.T,
        small_sum[:kernel_len],
        small_sum[kernel_len],
        small_sum[kernel_len + 1],
    )


def solution(mesh):
    return jax.shard_map(
        shards,
        mesh=mesh,
        in_specs=(
            P("sp", None),
            P("sp", None),
            P(None, "tp"),
            P(None, "tp"),
            P(None, "tp"),
            P("tp"),
            P("tp"),
            P("tp", None),
        ),
        out_specs=(
            P("sp", "tp"),
            P("sp", "tp"),
            P("sp", "tp"),
            P("tp", "sp"),
            P(None, "tp"),
            P("tp"),
            P("tp"),
        ),
        check_vma=False,
    )
```

```python
import functools
import math

import jax
import jax.numpy as jnp
from jax import lax
from jax.experimental import pallas as pl
from jax.experimental.pallas import tpu as pltpu
from jax.sharding import PartitionSpec as P

CH = 1024


EPS = 0.05


def from_behind(block, axis, distance):
    devices = range(lax.axis_size(axis))
    route = [(i - distance, i) for i in devices if i - distance in devices]
    return lax.ppermute(block, axis, route)


def right_product(left, right):
    return lax.dot_general(
        left, right, (((1,), (1,)), ((), ())), preferred_element_type=jnp.float32
    )


def column_product(left, right):
    return lax.dot_general(
        left, right, (((0,), (0,)), ((), ())), preferred_element_type=jnp.float32
    )


MESH = pl.DeviceIdType.MESH


def tail_kernel(
    n, n_tp, loss_scale,
    bi, og_hbm, wv, wg, gb_ref, mo_ref, small_ref,
    ig_ref, wv_out, wg_out, ps_out, taps_out, gain_out, shift_out,
    ws_ref, ps_ref, og, og_sem,
    gs, gr, gs2, gq, pm, pr, ps2, pq,
    xs, xr, ys, yr, acc, small_pair, small_in, small_all,
    gs_send, gs_recv, gq_send, gq_recv, pr_send, pr_recv, pq_send, pq_recv,
    x_send, x_recv, y_send, y_recv, s_send, s_recv, sa_send, sa_recv,
):
    me, t = lax.axis_index("sp"), lax.axis_index("tp")
    outer, inner = me // 2, me % 2
    h = n // 2
    mate = 2 * outer + (1 - inner)
    t_near, t_far = t + 1 - 2 * (t % 2), lax.rem(t + n_tp // 2, n_tp)
    t_cross = lax.rem(t_near + n_tp // 2, n_tp)
    rows = bi.shape[1] // n
    tokens = bi.shape[0]
    cols = bi.shape[1] // n_tp
    chans = mo_ref.shape[1]
    chunks = xs.shape[0]
    step = tokens // chunks

    og_load = pltpu.make_async_copy(og_hbm, og, og_sem.at[0])
    og_load.start()

    barrier = pltpu.get_barrier_semaphore()
    peers = [{"sp": 2 * lax.rem(outer + k, h) + inner} for k in range(1, h)]
    for who in peers + [{"sp": mate}, {"tp": t_near}, {"tp": t_far}]:
        pl.semaphore_signal(barrier, inc=1, device_id=who, device_id_type=MESH)
    pl.semaphore_wait(barrier, len(peers) + 3)

    def send(src, dst, send_sem, recv_sem, who):
        copy = pltpu.make_async_remote_copy(
            src_ref=src, dst_ref=dst, send_sem=send_sem, recv_sem=recv_sem,
            device_id=who, device_id_type=MESH,
        )
        copy.start()
        return copy

    small_copy = send(small_ref, small_in, s_send.at[0], s_recv.at[0], {"sp": mate})

    aligned = rows % 128 == 0
    wide = 256
    def block_rows(o, i):
        return pl.ds(pl.multiple_of((2 * o + i) * rows, rows), rows)

    def product(act, other, where):
        return lax.dot_general(
            act[:, where], other[...], (((0,), (0,)), ((), ())),
            preferred_element_type=jnp.float32,
        ).astype(jnp.bfloat16)

    def make_block(store, act, other, o, i):
        if aligned:
            store[block_rows(o, i), :] = product(act, other, block_rows(o, i))

    def make_all(store, act, other):
        if not aligned:
            for c in range(act.shape[1] // wide):
                where = pl.ds(c * wide, wide)
                store[where, :] = product(act, other, where)

    def partial_input(r, j):
        at = pl.ds(pl.multiple_of(j * cols, cols), cols)
        token = pl.ds(r * step, step)
        return right_product(gb_ref[token, :chans], wv[at, :]) + right_product(
            gb_ref[token, chans:], wg[at, :]
        )

    order = [lax.rem(outer + k, h) for k in range(1, h)] + [outer]

    def near_block(r):
        xs[r, 0] = partial_input(r, t_near).astype(jnp.bfloat16)
        xs[r, 1] = partial_input(r, t_cross).astype(jnp.bfloat16)
        return send(xs.at[r], xr.at[r], x_send.at[r], x_recv.at[r], {"tp": t_near})

    def far_block(r):
        mine = partial_input(r, t)
        far = partial_input(r, t_far)
        x_copies[r].wait_recv()
        ys[r] = (far + xr[r, 1].astype(jnp.float32)).astype(jnp.bfloat16)
        acc[pl.ds(r * step, step), :] = mine + xr[r, 0].astype(jnp.float32)
        return send(ys.at[r], yr.at[r], y_send.at[r], y_recv.at[r], {"tp": t_far})

    make_all(gs, bi, gb_ref)
    g_copies = []
    x_copies = []
    y_copies = []

    def g_block(k):
        o = order[k]
        make_block(gs, bi, gb_ref, o, 1 - inner)
        where = block_rows(o, 1 - inner)
        g_copies.append(send(gs.at[where], gr.at[k], gs_send.at[k], gs_recv.at[k], {"sp": mate}))

    g_block(0)
    x_copies.append(near_block(0))
    g_block(1)
    x_copies.append(near_block(1))
    y_copies.append(far_block(0))
    og_load.wait()
    make_all(pm, og, mo_ref)
    p_copies = []
    for k in range(h - 1):
        o = order[k]
        for i in range(2):
            make_block(pm, og, mo_ref, o, i)
        where = pl.ds(pl.multiple_of(2 * o * rows, 2 * rows), 2 * rows)
        p_copies.append(send(pm.at[where], pr.at[k], pr_send.at[k], pr_recv.at[k], {"sp": 2 * o + inner}))
        if k + 2 < h:
            g_block(k + 2)
    for r in range(2, chunks):
        x_copies.append(near_block(r))
        y_copies.append(far_block(r - 1))
    y_copies.append(far_block(chunks - 1))
    for i in range(2):
        make_block(pm, og, mo_ref, outer, i)
    small_copy.wait()
    small_pair[...] = small_ref[...] + small_in[...]
    sa_copies = [
        send(small_pair, small_all.at[outer], sa_send.at[k - 1], sa_recv.at[k - 1],
             {"sp": 2 * lax.rem(outer + k, h) + inner})
        for k in range(1, h)
    ]
    q_copies = []
    for k in range(h):
        o = order[k]
        make_block(gs, bi, gb_ref, o, inner)
        g_copies[k].wait_recv()
        total = gs[block_rows(o, inner), :].astype(jnp.float32) + gr[k].astype(jnp.float32)
        if k < h - 1:
            gs2[k] = total.astype(jnp.bfloat16)
            q_copies.append(send(gs2.at[k], gq.at[k], gq_send.at[k], gq_recv.at[k], {"sp": 2 * o + inner}))
        else:
            ws_ref[...] = total
    for copy in p_copies:
        copy.wait_recv()

    def proj_total(i):
        total = pm[block_rows(outer, i), :].astype(jnp.float32)
        for k in range(h - 1):
            total = total + pr[k, pl.ds(pl.multiple_of(i * rows, rows), rows), :].astype(jnp.float32)
        return total

    ps2[...] = proj_total(1 - inner).astype(jnp.bfloat16)
    last = send(ps2, pq, pq_send.at[0], pq_recv.at[0], {"sp": mate})
    ps_ref[...] = proj_total(inner)
    for copy in sa_copies:
        copy.wait_recv()
    small_all[outer] = small_pair[...]
    total = small_all[0]
    for k in range(1, h):
        total = total + small_all[k]
    total = total * loss_scale
    taps = taps_out.shape[0]
    taps_out[...] = total[:taps]
    gain_out[...] = total[taps : taps + 1]
    shift_out[...] = total[taps + 1 : taps + 2]
    for r in range(chunks):
        y_copies[r].wait_recv()
        token = pl.ds(r * step, step)
        ig_ref[token, :] = (acc[token, :] + yr[r].astype(jnp.float32)).astype(jnp.bfloat16)
    for copy in q_copies:
        copy.wait_recv()
    total = ws_ref[...]
    for k in range(h - 1):
        total = total + gq[k].astype(jnp.float32)
    wv_out[...] = total[:, :chans] * loss_scale
    wg_out[...] = total[:, chans:] * loss_scale
    last.wait_recv()
    total = (ps_ref[...] + pq[...].astype(jnp.float32)) * loss_scale
    ps_out[...] = total.T if aligned else total
    for copy in g_copies + x_copies + y_copies + p_copies + q_copies + sa_copies + [last]:
        copy.wait_send()


def tail(block_input, out_grad, w_value, w_gate, grad_both, mixer_out, small, taps, loss_scale):
    n, n_tp = lax.axis_size("sp"), lax.axis_size("tp")
    tokens, width = block_input.shape
    chans = mixer_out.shape[1]
    rows, cols, h, chunks = width // n, width // n_tp, n // 2, 4
    step = tokens // chunks
    bf, f32 = jnp.bfloat16, jnp.float32
    vmem = pl.BlockSpec(memory_space=pltpu.VMEM)
    dma = pltpu.SemaphoreType.DMA
    V = pltpu.VMEM
    return pl.pallas_call(
        functools.partial(tail_kernel, n, n_tp, loss_scale),
        out_shape=(
            jax.ShapeDtypeStruct((tokens, cols), bf),
            jax.ShapeDtypeStruct((rows, chans), f32),
            jax.ShapeDtypeStruct((rows, chans), f32),
            jax.ShapeDtypeStruct((chans, rows) if rows % 128 == 0 else (rows, chans), f32),
            jax.ShapeDtypeStruct((taps, chans), f32),
            jax.ShapeDtypeStruct((1, chans), f32),
            jax.ShapeDtypeStruct((1, chans), f32),
        ),
        in_specs=[vmem, pl.BlockSpec(memory_space=pltpu.HBM)] + [vmem] * 5,
        out_specs=(vmem,) * 7,
        scratch_shapes=[
            V((rows, 2 * chans), f32), V((rows, chans), f32), V((tokens, width), bf), dma((1,)),
            V((width, 2 * chans), bf), V((h, rows, 2 * chans), bf), V((h - 1, rows, 2 * chans), bf),
            V((h - 1, rows, 2 * chans), bf),
            V((width, chans), bf), V((h - 1, 2 * rows, chans), bf), V((rows, chans), bf), V((rows, chans), bf),
            V((chunks, 2, step, cols), bf), V((chunks, 2, step, cols), bf), V((chunks, step, cols), bf),
            V((chunks, step, cols), bf), V((tokens, cols), f32),
            V(small.shape, f32), V(small.shape, f32), V((h,) + small.shape, f32),
            dma((h,)), dma((h,)), dma((h - 1,)), dma((h - 1,)), dma((h - 1,)), dma((h - 1,)), dma((1,)), dma((1,)),
            dma((chunks,)), dma((chunks,)), dma((chunks,)), dma((chunks,)), dma((1,)), dma((1,)),
            dma((h - 1,)), dma((h - 1,)),
        ],
        compiler_params=pltpu.CompilerParams(
            collective_id=0, has_side_effects=True, vmem_limit_bytes=36 * 1024 * 1024
        ),
    )(block_input, out_grad, w_value, w_gate, grad_both, mixer_out, small)


def shards(block_input, out_grad, w_value, w_gate, conv_taps, norm_gain, norm_shift, w_proj):
    tok_rows = block_input.shape[0]
    kernel_len = conv_taps.shape[0]
    reach_back = kernel_len - 1
    channels_dev = w_value.shape[1]
    loss_scale = 1.0 / math.sqrt(tok_rows * lax.axis_size("sp"))
    value_proj = jnp.dot(block_input, w_value, preferred_element_type=jnp.float32).astype(
        jnp.bfloat16
    )
    gate_proj = jnp.dot(block_input, w_gate, preferred_element_type=jnp.float32).astype(
        jnp.bfloat16
    )
    gate_sigmoid = jax.nn.sigmoid(gate_proj.astype(jnp.float32))
    value_wide = value_proj.astype(jnp.float32)
    gated_input = (value_wide * gate_sigmoid).astype(jnp.bfloat16)
    earlier = from_behind(gated_input[tok_rows - reach_back :], "sp", 1)
    extended = jnp.concatenate([earlier, gated_input], axis=0).astype(jnp.float32)
    filtered = jnp.zeros((tok_rows, channels_dev), jnp.float32)
    for tap_index in range(kernel_len):
        begin = reach_back - tap_index
        filtered = filtered + conv_taps[tap_index] * extended[begin : begin + tok_rows]
    row_sum, row_square = lax.psum(
        (jnp.sum(filtered, axis=1), jnp.sum(filtered * filtered, axis=1)), "tp"
    )
    row_mean = row_sum / CH
    row_var = row_square / CH - row_mean * row_mean
    row_scale = lax.rsqrt(row_var + EPS)
    normed = (filtered - row_mean[:, None]) * row_scale[:, None]
    activated = normed * norm_gain + norm_shift
    act_sigmoid = jax.nn.sigmoid(activated)
    mixer_out = (activated * act_sigmoid).astype(jnp.bfloat16)
    grad_mixed = right_product(out_grad, w_proj)
    grad_act = grad_mixed * act_sigmoid * (1.0 + activated * (1.0 - act_sigmoid))
    grad_normed = grad_act * norm_gain
    back_sum, back_cross = lax.psum(
        (jnp.sum(grad_normed, axis=1), jnp.sum(grad_normed * normed, axis=1)), "tp"
    )
    grad_filtered = row_scale[:, None] * (
        grad_normed - back_sum[:, None] / CH - normed * (back_cross[:, None] / CH)
    )
    gain_part = jnp.sum(grad_act * normed, axis=0)
    shift_part = jnp.sum(grad_act, axis=0)
    padded_grad = jnp.pad(grad_filtered, ((reach_back, reach_back), (0, 0)))
    grad_extended = jnp.zeros((tok_rows + reach_back, channels_dev), jnp.float32)
    taps_rows = []
    for tap_index in range(kernel_len):
        begin = reach_back - tap_index
        grad_extended = (
            grad_extended
            + conv_taps[tap_index] * padded_grad[tap_index : tap_index + tok_rows + reach_back]
        )
        taps_rows.append(jnp.sum(grad_filtered * extended[begin : begin + tok_rows], axis=0))
    taps_part = jnp.stack(taps_rows, axis=0)
    returned = from_behind(grad_extended[:reach_back], "sp", -1)
    grad_glu = jnp.concatenate(
        [grad_extended[reach_back:tok_rows], grad_extended[tok_rows:] + returned], axis=0
    )
    grad_value = (grad_glu * gate_sigmoid).astype(jnp.bfloat16)
    grad_gate = (grad_glu * value_wide * gate_sigmoid * (1.0 - gate_sigmoid)).astype(jnp.bfloat16)
    grad_both = jnp.concatenate([grad_value, grad_gate], axis=1)
    small = jnp.concatenate([taps_part, gain_part[None], shift_part[None]], axis=0)
    small = jnp.pad(small, ((0, -small.shape[0] % 8), (0, 0)))
    input_grad, value_wgrad, gate_wgrad, proj_wgrad, taps_grad, gain_grad, shift_grad = tail(
        block_input, out_grad, w_value, w_gate, grad_both, mixer_out, small, kernel_len, loss_scale
    )
    if proj_wgrad.shape[0] != channels_dev:
        proj_wgrad = proj_wgrad.T
    return (
        input_grad, value_wgrad, gate_wgrad, proj_wgrad, taps_grad,
        gain_grad.reshape(channels_dev), shift_grad.reshape(channels_dev),
    )


def solution(mesh):
    return jax.shard_map(
        shards,
        mesh=mesh,
        in_specs=(
            P("sp", None),
            P("sp", None),
            P(None, "tp"),
            P(None, "tp"),
            P(None, "tp"),
            P("tp"),
            P("tp"),
            P("tp", None),
        ),
        out_specs=(
            P("sp", "tp"),
            P("sp", "tp"),
            P("sp", "tp"),
            P("tp", "sp"),
            P(None, "tp"),
            P("tp"),
            P("tp"),
        ),
        check_vma=False,
    )
```
